32 devices in a mesh: sp: 16 (over z, y, x), tp: 2 (over core).
Axes of the slice: x: 2, y: 2, z: 4, core: 2. Of those that a mesh axis runs over, the one named last changes fastest.
Arguments:
- queries: bfloat16 [3, 4096, 2048], P(None, 'sp', 'tp'), may hold values from -6 to 6
- keys: bfloat16 [3, 4096, 2048], P(None, 'sp', 'tp'), may hold values from -6 to 6
- values: bfloat16 [3, 4096, 2048], P(None, 'sp', 'tp'), may hold values from -6 to 6
- w_out: bfloat16 [2048, 2048], P(None, 'tp'), may hold values from -1 to 1
Outputs:
- mixed: bfloat16 [4096, 2048], P('sp', 'tp')
The draws below stay inside these ranges and needn't reach their ends.
All inputs are finite; a program needn't handle non-finite values.
Results may differ from the reference program's by a relative error of at most 0.01.
Values may be sent and summed in bfloat16 or wider, within the bound.
A program may use at most 128 MiB of HBM per device.

```python
from functools import partial
import jax
import jax.numpy as jnp
from jax import lax

D = 2048
HEADS = 16
HEAD = 128
GROUPS = 3
KEYS_PER_QUERY = 128
FIRST_STRIDE = 1
SECOND_STRIDE = 4
THIRD_STRIDE = 16
TOKENS = 4096


def planted_pair(key):
    base = jax.random.fold_in(key, 11)
    first_key, second_key, pick_key, sign_key = jax.random.split(base, 4)
    shape = (GROUPS, TOKENS, HEADS * HEAD)
    query_part = jnp.clip(jax.random.normal(first_key, shape, jnp.float32), -6.0, 6.0)
    key_part = jnp.clip(jax.random.normal(second_key, shape, jnp.float32), -6.0, 6.0)
    return (query_part, key_part)


def draw_queries(key, part):
    return planted_pair(key)[0].astype(jnp.bfloat16)


def draw_keys(key, part):
    return planted_pair(key)[1].astype(jnp.bfloat16)


def block_levels(stream_key, extent, cuts, least, top_value):
    gain = 1.0
    for axis_at, parts in cuts:
        steps = jax.random.uniform(jax.random.fold_in(jax.random.fold_in(stream_key, 6), axis_at), (parts,), jnp.float32, least / len(cuts), top_value / len(cuts))
        gain = gain * jnp.repeat(jnp.exp(steps), extent[axis_at] // parts).reshape((-1,) + (1,) * (len(extent) - 1 - axis_at))
    return gain


def bell_draw(key, extent, scale, bound, shards=(), held_as=jnp.bfloat16):
    values = jax.random.normal(key, extent, jnp.float32) * scale
    if len(shards) > 0:
        values = block_levels(key, extent, shards, -0.22, 0.18) * values
    return jnp.clip(values, min=-bound, max=bound).astype(held_as)


def setup_inputs(seed: int = 0) -> dict:
    splits = jax.random.split(jax.random.key(seed), 5)
    queries = draw_queries(jax.random.fold_in(splits[4], 71), 0)
    keys = draw_keys(jax.random.fold_in(splits[4], 71), 0)
    values = bell_draw(splits[2], (GROUPS, TOKENS, HEADS * HEAD), 1.0, 6.0, ((1, 16), (2, 2)))
    w_out = bell_draw(splits[3], (HEADS * HEAD, D), (HEADS * HEAD // 64) ** -0.5, 1.0, ((1, 2),))
    return {"queries": queries, "keys": keys, "values": values, "w_out": w_out}


ROPE_BASE = 10000.0
MASKED = -1e30


def turn_halves(matrix, cosine, sine_part):
    first_half, second_half = jnp.split(matrix, 2, axis=-1)
    return jnp.concatenate([first_half * cosine - second_half * sine_part,
                            second_half * cosine + first_half * sine_part], axis=-1)


def strided_head(triple, dilation):
    query_head, key_head, value_head = triple
    length = query_head.shape[0]
    block_count = length // (KEYS_PER_QUERY * dilation)

    def blocked(matrix):
        shaped = jnp.transpose(matrix.reshape(length // dilation, dilation, HEAD), (1, 0, 2))
        return shaped.reshape(dilation, block_count, KEYS_PER_QUERY, HEAD).astype(jnp.float32)

    def with_previous(matrix):
        shaped = blocked(matrix)
        earlier = jnp.concatenate([jnp.zeros_like(shaped[:, :1]), shaped[:, :-1]], axis=1)
        return jnp.concatenate([earlier, shaped], axis=2)

    q_blocks = blocked(query_head)
    key_blocks = with_previous(key_head)
    value_blocks = with_previous(value_head)
    scores = jnp.einsum("dnqe,dnke->dnqk", q_blocks, key_blocks, precision=lax.Precision.HIGHEST)
    q_index = jnp.arange(KEYS_PER_QUERY)[:, None]
    k_index = jnp.arange(2 * KEYS_PER_QUERY)[None, :]
    distance = q_index + KEYS_PER_QUERY - k_index
    band = (distance >= 0) & (distance <= KEYS_PER_QUERY)
    opening = (jnp.arange(block_count)[:, None, None] == 0) & (k_index[None] < KEYS_PER_QUERY)
    allowed = band[None] & jnp.logical_not(opening)
    scores = jnp.where(allowed[None], scores, MASKED)
    row_max = jnp.max(scores, axis=-1, keepdims=True)
    weights = jnp.exp(scores - row_max)
    row_sum = jnp.sum(weights, axis=-1, keepdims=True)
    rounded = lax.optimization_barrier(weights.astype(jnp.bfloat16)).astype(jnp.float32)
    weighted = jnp.einsum("dnqk,dnke->dnqe", rounded, value_blocks, precision=lax.Precision.HIGHEST)
    result = weighted / row_sum
    log_sum = (row_max + jnp.log(row_sum))[..., 0]
    result = jnp.transpose(result.reshape(dilation, length // dilation, HEAD), (1, 0, 2)).reshape(length, HEAD)
    log_sum = jnp.transpose(log_sum.reshape(dilation, length // dilation)).reshape(length)
    return result, log_sum


def reference(queries, keys, values, w_out):
    length = queries.shape[1]
    positions = jnp.arange(length, dtype=jnp.int32).astype(jnp.float32)
    inverse = ROPE_BASE ** (-jnp.arange(0, HEAD, 2, dtype=jnp.float32) / HEAD)
    angles = positions[:, None] * inverse[None, :]
    cosine = jnp.cos(angles)[:, None, :]
    sine_part = jnp.sin(angles)[:, None, :]
    group_strides = (FIRST_STRIDE, SECOND_STRIDE, THIRD_STRIDE)
    results = []
    log_sums = []
    for group_id in range(len(group_strides)):
        query_f = queries[group_id].astype(jnp.float32).reshape(length, HEADS, HEAD)
        key_f = keys[group_id].astype(jnp.float32).reshape(length, HEADS, HEAD)
        turned_q = (turn_halves(query_f, cosine, sine_part) * HEAD ** -0.5).astype(jnp.bfloat16)
        turned_k = turn_halves(key_f, cosine, sine_part).astype(jnp.bfloat16)
        value_h = values[group_id].reshape(length, HEADS, HEAD)
        result, log_sum = lax.map(partial(strided_head, dilation=group_strides[group_id]),
                                  (jnp.transpose(turned_q, (1, 0, 2)),
                                   jnp.transpose(turned_k, (1, 0, 2)),
                                   jnp.transpose(value_h, (1, 0, 2))))
        results.append(jnp.transpose(result, (1, 0, 2)))
        log_sums.append(jnp.transpose(log_sum))
    shares = jax.nn.softmax(jnp.stack(log_sums), axis=0)
    attended = jnp.sum(shares[..., None] * jnp.stack(results), axis=0)
    attended = attended.astype(jnp.bfloat16).reshape(length, HEADS * HEAD)
    return jnp.dot(attended, w_out, preferred_element_type=jnp.float32).astype(jnp.bfloat16)
```

```python
import functools

import jax
import jax.numpy as jnp
from jax import lax
from jax.experimental import pallas as pl
from jax.experimental.pallas import tpu as pltpu
from jax.sharding import PartitionSpec as P

HEAD = 128
KEYS = 128
STRIDES = (1, 4, 16)
ROPE_BASE = 10000.0
MASKED = -1e30
TEAM = 4

MESH = pl.DeviceIdType.MESH
F32 = jnp.float32
BF16 = jnp.bfloat16


def kernel(
    cfg,
    q_in, k_in, v_in, w_in, cos_ref, sin_ref,
    o_ref,
    raw, ready, w_buf, tables, perms, q_buf, kv0, kv1, kv2, acc, top, den, att, full,
    in_sem, w_sem, deal_send, deal_recv, hop_send, hop_recv, ret_send, ret_recv, d2d_send, d2d_recv,
):
    tokens, n_sp, heads = cfg
    width = heads * HEAD
    mine = heads // TEAM
    part = mine * HEAD
    span = TEAM * tokens
    sp = lax.axis_index("sp")
    tp = lax.axis_index("tp")
    team = sp // TEAM
    me = lax.rem(sp, TEAM)
    has_next = sp + TEAM < n_sp
    has_prev = sp >= TEAM
    has_prev2 = sp >= 2 * TEAM

    inputs = (q_in, k_in, v_in)
    Q, K, V = 0, 1, 2
    order = [(V, 2), (K, 2), (V, 1), (K, 1), (V, 0), (K, 0), (Q, 1), (Q, 0), (Q, 2)]
    loads = {}
    for kind, g in order:
        copy = pltpu.make_async_copy(inputs[kind].at[g], raw.at[kind, g], in_sem.at[kind, g])
        copy.start()
        loads[kind, g] = copy
    w_copy = pltpu.make_async_copy(w_in, w_buf, w_sem)
    w_copy.start()

    barrier = pltpu.get_barrier_semaphore()
    for d in range(1, TEAM):
        peer = team * TEAM + lax.rem(me + d, TEAM)
        pl.semaphore_signal(barrier, inc=1, device_id={"sp": peer}, device_id_type=MESH)
    pl.semaphore_signal(barrier, inc=1, device_id={"tp": 1 - tp}, device_id_type=MESH)

    @pl.when(has_next)
    def _():
        pl.semaphore_signal(barrier, inc=1, device_id={"sp": sp + TEAM}, device_id_type=MESH)

    @pl.when(has_prev)
    def _():
        pl.semaphore_signal(barrier, inc=1, device_id={"sp": sp - TEAM}, device_id_type=MESH)

    row = lax.broadcasted_iota(jnp.int32, (tokens, tokens), 0)
    col = lax.broadcasted_iota(jnp.int32, (tokens, tokens), 1)
    for g in (1, 2):
        stride = STRIDES[g]
        each = tokens // stride
        origin = lax.rem(row, each) * stride + row // each
        perms[g - 1] = jnp.where(origin == col, 1.0, 0.0).astype(BF16)
    for g in range(3):
        stride = STRIDES[g]
        each = tokens // stride
        for r in range(stride):
            tables[0, g, r * each : (r + 1) * each, :] = cos_ref[pl.ds(r, each, stride=stride), :]
            tables[1, g, r * each : (r + 1) * each, :] = sin_ref[pl.ds(r, each, stride=stride), :]

    def prepare(kind, g):
        loads[kind, g].wait()

        def step(h, carry):
            lanes = pl.ds(pl.multiple_of(h * HEAD, HEAD), HEAD)
            x = raw[kind, g, :, lanes]
            if g > 0:
                x = jnp.dot(perms[g - 1], x, preferred_element_type=F32)
            else:
                x = x.astype(F32)
            if kind != V:
                x = x * tables[0, g] + pltpu.roll(x, HEAD // 2, 1) * tables[1, g]
            if kind == Q:
                x = x * HEAD ** (-0.5)
            ready[kind, g, :, lanes] = x.astype(BF16)
            return carry

        lax.fori_loop(0, heads, step, 0, unroll=2)

    def slot(kind, g, s):
        if kind == Q:
            return q_buf.at[g, s]
        if g == 2:
            return kv2.at[kind - 1, 2 * TEAM + s]
        if g == 1:
            return kv1.at[kind - 1, 2 + s]
        return kv0.at[kind - 1, pl.ds(pl.multiple_of(KEYS + s * tokens, KEYS), tokens)]

    def lanes_of(j):
        return pl.ds(pl.multiple_of(j * part, part), part)

    def deal(kind, g, d):
        peer = lax.rem(me + d, TEAM)
        return pltpu.make_async_remote_copy(
            src_ref=ready.at[kind, g, :, lanes_of(peer)],
            dst_ref=slot(kind, g, me),
            send_sem=deal_send.at[kind, g, d],
            recv_sem=deal_recv.at[kind, g, d],
            device_id={"sp": team * TEAM + peer},
            device_id_type=MESH,
        )

    def source(d):
        return lax.rem(me + TEAM - d, TEAM)

    def wait_deal(kind, g, d):
        here = slot(kind, g, source(d))
        pltpu.make_async_remote_copy(
            src_ref=here, dst_ref=here,
            send_sem=deal_send.at[kind, g, d], recv_sem=deal_recv.at[kind, g, d],
            device_id={"sp": team * TEAM + source(d)}, device_id_type=MESH,
        ).wait_recv()

    def hop(kind, index, src, dst):
        return pltpu.make_async_remote_copy(
            src_ref=src, dst_ref=dst,
            send_sem=hop_send.at[kind - 1, index], recv_sem=hop_recv.at[kind - 1, index],
            device_id={"sp": lax.rem(sp + TEAM, n_sp)}, device_id_type=MESH,
        )

    def first_hop(kind, s):
        return hop(kind, s, kv2.at[kind - 1, 2 * TEAM + s], kv2.at[kind - 1, TEAM + s])

    def second_hop(kind, s):
        return hop(kind, TEAM + s, kv2.at[kind - 1, TEAM + s], kv2.at[kind - 1, s])

    def near_hop(kind, i):
        return hop(kind, 2 * TEAM + i, kv1.at[kind - 1, TEAM + i], kv1.at[kind - 1, i])

    def edge_hop(kind):
        return hop(
            kind, 2 * TEAM + 2,
            kv0.at[kind - 1, pl.ds(span, KEYS)], kv0.at[kind - 1, pl.ds(0, KEYS)],
        )

    def forward(kind, g, s):
        if g == 2:
            pl.when(has_next)(lambda: first_hop(kind, s).start())
        elif g == 1:
            pl.when(has_next & (s >= TEAM - 2))(lambda: near_hop(kind, s - (TEAM - 2)).start())
        else:
            pl.when(has_next & (s == TEAM - 1))(lambda: edge_hop(kind).start())

    def relay(d):
        s = source(d)
        for kind in (V, K):

            @pl.when(has_prev)
            def _():
                first_hop(kind, s).wait_recv()

            @pl.when(has_prev & has_next)
            def _():
                second_hop(kind, s).start()

    def place(kind, g):
        slot(kind, g, me)[...] = ready[kind, g, :, lanes_of(me)]

    def arrive(g, d):
        for kind in (V, K):
            wait_deal(kind, g, d)
            forward(kind, g, source(d))

    barrier_waited = False
    for n, (kind, g) in enumerate(order):
        prepare(kind, g)
        place(kind, g)
        if not barrier_waited:
            count = TEAM + has_next.astype(jnp.int32) + has_prev.astype(jnp.int32)
            pl.semaphore_wait(barrier, count)
            barrier_waited = True
        for d in range(1, TEAM):
            deal(kind, g, d).start()
        if kind != Q:
            forward(kind, g, me)
        if n == 3:
            arrive(2, 1)
        if n == 5:
            arrive(2, 2)
    arrive(2, 3)
    relay(0)
    relay(1)
    for d in range(1, TEAM):
        arrive(1, d)
    relay(2)
    relay(3)
    for d in range(1, TEAM):
        arrive(0, d)

    @pl.when(jnp.logical_not(has_prev))
    def _():
        for kind in range(2):
            kv0[kind, 0:KEYS, :] = jnp.zeros((KEYS, part), BF16)
            for s in range(2):
                kv1[kind, s] = jnp.zeros((tokens, part), BF16)
            for s in range(TEAM):
                kv2[kind, TEAM + s] = jnp.zeros((tokens, part), BF16)

    @pl.when(jnp.logical_not(has_prev2))
    def _():
        for kind in range(2):
            for s in range(TEAM):
                kv2[kind, s] = jnp.zeros((tokens, part), BF16)

    def attend(g, head, query, key, value, index, start):
        rows, seen = query.shape[0], key.shape[0]
        a = lax.broadcasted_iota(jnp.int32, (rows, seen), 0)
        b = lax.broadcasted_iota(jnp.int32, (rows, seen), 1)
        allowed = (b >= jnp.maximum(a, KEYS - index)) & (b <= a + KEYS)
        scores = lax.dot_general(
            query, key, (((1,), (1,)), ((), ())), preferred_element_type=F32
        )
        scores = jnp.where(allowed, scores, MASKED)
        best = jnp.max(scores, axis=1, keepdims=True)
        weights = jnp.exp(scores - best)
        total = jnp.sum(weights, axis=1, keepdims=True)
        out = jnp.dot(weights.astype(BF16), value, preferred_element_type=F32)
        where = pl.ds(start, rows, stride=STRIDES[g]) if g else pl.ds(start, rows)
        acc[g, head, where, :] = out
        top[g, head, where, :] = jnp.broadcast_to(best, (rows, HEAD))
        den[g, head, where, :] = jnp.broadcast_to(total, (rows, HEAD))

    def cols(head):
        return slice(head * HEAD, (head + 1) * HEAD)

    for d in range(1, TEAM):
        wait_deal(Q, 1, d)

    @pl.when(has_prev)
    def _():
        for kind in (V, K):
            for i in range(2):
                near_hop(kind, i).wait_recv()

    each = tokens // STRIDES[1]
    pair = KEYS // each

    def step1(n, carry):
        r, i = n // (TEAM // pair), lax.rem(n, TEAM // pair)
        rows = pl.ds(pl.multiple_of(r * each, each), each)
        for head in range(mine):
            query = q_buf[1, pl.ds(i * pair, pair), rows, cols(head)].reshape(KEYS, HEAD)
            key = kv1[0, pl.ds(i * pair, 2 * pair), rows, cols(head)].reshape(2 * KEYS, HEAD)
            value = kv1[1, pl.ds(i * pair, 2 * pair), rows, cols(head)].reshape(2 * KEYS, HEAD)
            attend(1, head, query, key, value,
                   team * (span // STRIDES[1]) + i * KEYS, r + STRIDES[1] * KEYS * i)
        return carry

    lax.fori_loop(0, STRIDES[1] * (TEAM // pair), step1, 0, unroll=2)

    for d in range(1, TEAM):
        wait_deal(Q, 0, d)

    @pl.when(has_prev)
    def _():
        for kind in (V, K):
            edge_hop(kind).wait_recv()

    per = tokens // KEYS

    def step0(n, carry):
        inner = pl.ds(pl.multiple_of(lax.rem(n, per) * KEYS, KEYS), KEYS)
        rows = pl.ds(pl.multiple_of(n * KEYS, KEYS), 2 * KEYS)
        for head in range(mine):
            query = q_buf[0, n // per, inner, cols(head)]
            attend(0, head, query, kv0[0, rows, cols(head)], kv0[1, rows, cols(head)],
                   team * span + n * KEYS, pl.multiple_of(n * KEYS, KEYS))
        return carry

    lax.fori_loop(0, span // KEYS, step0, 0, unroll=2)

    for d in range(1, TEAM):
        wait_deal(Q, 2, d)

    @pl.when(has_prev2)
    def _():
        for d in range(TEAM):
            for kind in (V, K):
                second_hop(kind, source(d)).wait_recv()

    few = tokens // STRIDES[2]

    def step2(r, carry):
        rows = pl.ds(pl.multiple_of(r * few, few), few)
        for head in range(mine):
            query = q_buf[2, :, rows, cols(head)].reshape(TEAM * few, HEAD)
            key = kv2[0, :, rows, cols(head)].reshape(3 * TEAM * few, HEAD)
            value = kv2[1, :, rows, cols(head)].reshape(3 * TEAM * few, HEAD)
            attend(2, head, query, key, value, team * (span // STRIDES[2]), r)
        return carry

    lax.fori_loop(0, STRIDES[2], step2, 0, unroll=2)

    def merge(j):
        rows = pl.ds(pl.multiple_of(j * tokens, tokens), tokens)
        for head in range(mine):
            peak = jnp.maximum(
                jnp.maximum(top[0, head, rows, :], top[1, head, rows, :]), top[2, head, rows, :]
            )
            upper = jnp.zeros((tokens, HEAD), F32)
            lower = jnp.zeros((tokens, HEAD), F32)
            for g in range(3):
                scale = jnp.exp(top[g, head, rows, :] - peak)
                upper = upper + scale * acc[g, head, rows, :]
                lower = lower + scale * den[g, head, rows, :]
            att[j, :, cols(head)] = (upper / lower).astype(BF16)

    def home(d):
        peer = lax.rem(me + d, TEAM)
        return pltpu.make_async_remote_copy(
            src_ref=att.at[peer], dst_ref=full.at[tp, me],
            send_sem=ret_send.at[d], recv_sem=ret_recv.at[d],
            device_id={"sp": team * TEAM + peer}, device_id_type=MESH,
        )

    def twin(d, half):
        here = full.at[half, source(d)]
        return pltpu.make_async_remote_copy(
            src_ref=here, dst_ref=here,
            send_sem=d2d_send.at[d], recv_sem=d2d_recv.at[d],
            device_id={"tp": 1 - tp}, device_id_type=MESH,
        )

    for d in (2, 1, 3, 0):
        merge(lax.rem(me + d, TEAM))
        if d:
            home(d).start()
    full[tp, me] = att[me]
    twin(0, tp).start()
    w_copy.wait()

    def project(half, s):
        start = pl.multiple_of(half * width + s * part, part)
        return jnp.dot(full[half, s], w_buf[pl.ds(start, part), :], preferred_element_type=F32)

    result = acc_view = None
    total = project(tp, me)
    for d in (1, 3, 2):
        here = full.at[tp, source(d)]
        pltpu.make_async_remote_copy(
            src_ref=here, dst_ref=here, send_sem=ret_send.at[d], recv_sem=ret_recv.at[d],
            device_id={"sp": team * TEAM + source(d)}, device_id_type=MESH,
        ).wait_recv()
        twin(d, tp).start()
        total = total + project(tp, source(d))
    for d in (0, 1, 3, 2):
        twin(d, 1 - tp).wait_recv()
        total = total + project(1 - tp, source(d))
    o_ref[...] = total.astype(BF16)

    for kind, g in order:
        for d in range(1, TEAM):
            deal(kind, g, d).wait_send()
    for d in range(1, TEAM):
        home(d).wait_send()
    for d in range(TEAM):
        twin(d, tp).wait_send()

    @pl.when(has_next)
    def _():
        for kind in (V, K):
            for s in range(TEAM):
                first_hop(kind, s).wait_send()
            for i in range(2):
                near_hop(kind, i).wait_send()
            edge_hop(kind).wait_send()

    @pl.when(has_prev & has_next)
    def _():
        for kind in (V, K):
            for s in range(TEAM):
                second_hop(kind, s).wait_send()


def shards(n_sp, queries, keys, values, w_out):
    tokens, width = queries.shape[1:]
    heads = width // HEAD
    mine = heads // TEAM
    part = mine * HEAD
    span = TEAM * tokens
    start = lax.axis_index("sp") * tokens
    positions = (lax.iota(jnp.int32, tokens) + start).astype(F32)
    inverse = ROPE_BASE ** (-jnp.arange(0, HEAD, 2, dtype=F32) / HEAD)
    angles = positions[:, None] * inverse[None, :]
    cosine, sine = jnp.cos(angles), jnp.sin(angles)
    cosine = jnp.concatenate([cosine, cosine], axis=1)
    sine = jnp.concatenate([-sine, sine], axis=1)
    any_spec = pl.BlockSpec(memory_space=pl.ANY)
    vmem = pl.BlockSpec(memory_space=pltpu.VMEM)
    dma = pltpu.SemaphoreType.DMA
    return pl.pallas_call(
        functools.partial(kernel, (tokens, n_sp, heads)),
        out_shape=jax.ShapeDtypeStruct((tokens, w_out.shape[1]), BF16),
        in_specs=[any_spec] * 4 + [vmem] * 2,
        out_specs=vmem,
        scratch_shapes=[
            pltpu.VMEM((3, 3, tokens, width), BF16),
            pltpu.VMEM((3, 3, tokens, width), BF16),
            pltpu.VMEM(w_out.shape, BF16),
            pltpu.VMEM((2, 3, tokens, HEAD), F32),
            pltpu.VMEM((2, tokens, tokens), BF16),
            pltpu.VMEM((3, TEAM, tokens, part), BF16),
            pltpu.VMEM((2, KEYS + span, part), BF16),
            pltpu.VMEM((2, 2 + TEAM, tokens, part), BF16),
            pltpu.VMEM((2, 3 * TEAM, tokens, part), BF16),
            pltpu.VMEM((3, mine, span, HEAD), F32),
            pltpu.VMEM((3, mine, span, HEAD), F32),
            pltpu.VMEM((3, mine, span, HEAD), F32),
            pltpu.VMEM((TEAM, tokens, part), BF16),
            pltpu.VMEM((2, TEAM, tokens, part), BF16),
            dma((3, 3)),
            dma,
            dma((3, 3, TEAM)),
            dma((3, 3, TEAM)),
            dma((2, 2 * TEAM + 3)),
            dma((2, 2 * TEAM + 3)),
            dma((TEAM,)),
            dma((TEAM,)),
            dma((TEAM,)),
            dma((TEAM,)),
        ],
        compiler_params=pltpu.CompilerParams(
            collective_id=0, has_side_effects=True, vmem_limit_bytes=60 * 1024 * 1024
        ),
    )(queries, keys, values, w_out, cosine, sine)


def solution(mesh):
    return jax.shard_map(
        functools.partial(shards, mesh.shape["sp"]),
        mesh=mesh,
        in_specs=(P(None, "sp", "tp"), P(None, "sp", "tp"), P(None, "sp", "tp"), P(None, "tp")),
        out_specs=P("sp", "tp"),
        check_vma=False,
    )
```

```python
import functools

import jax
import jax.numpy as jnp
from jax import lax
from jax.experimental import pallas as pl
from jax.experimental.pallas import tpu as pltpu
from jax.sharding import PartitionSpec as P

HEAD = 128
KEYS = 128
STRIDES = (1, 4, 16)
ROPE_BASE = 10000.0
MASKED = -1e30
TEAM = 4

MESH = pl.DeviceIdType.MESH
F32 = jnp.float32
BF16 = jnp.bfloat16


def kernel(
    cfg,
    q_in, k_in, v_in, w_in, cos_ref, sin_ref,
    o_ref,
    raw, ready, w_buf, tables, perms, q_buf, kv0, kv1, kv2, acc, lse, bias, att, full, total_buf,
    in_sem, w_sem, deal_send, deal_recv, hop_send, hop_recv, ret_send, ret_recv, d2d_send, d2d_recv,
):
    tokens, n_sp, heads = cfg
    width = heads * HEAD
    mine = heads // TEAM
    part = mine * HEAD
    span = TEAM * tokens
    sp = lax.axis_index("sp")
    tp = lax.axis_index("tp")
    team = sp // TEAM
    me = lax.rem(sp, TEAM)
    has_next = sp + TEAM < n_sp
    has_prev = sp >= TEAM
    has_prev2 = sp >= 2 * TEAM

    inputs = (q_in, k_in, v_in)
    Q, K, V = 0, 1, 2
    order = [(V, 2), (K, 2), (V, 1), (K, 1), (V, 0), (K, 0), (Q, 1), (Q, 0), (Q, 2)]
    loads = {}
    for kind, g in order:
        copy = pltpu.make_async_copy(inputs[kind].at[g], raw.at[kind, g], in_sem.at[kind, g])
        copy.start()
        loads[kind, g] = copy
    w_loads = []
    for half in range(2):
        for head in range(mine):
            for s in range(TEAM):
                rows = pl.ds(half * width + s * part + head * HEAD, HEAD)
                copy = pltpu.make_async_copy(
                    w_in.at[rows],
                    w_buf.at[half, head, pl.ds(s * HEAD, HEAD)],
                    w_sem.at[half, head, s],
                )
                copy.start()
                w_loads.append(copy)

    barrier = pltpu.get_barrier_semaphore()
    for d in range(1, TEAM):
        peer = team * TEAM + lax.rem(me + d, TEAM)
        pl.semaphore_signal(barrier, inc=1, device_id={"sp": peer}, device_id_type=MESH)
    pl.semaphore_signal(barrier, inc=1, device_id={"tp": 1 - tp}, device_id_type=MESH)

    @pl.when(has_next)
    def _():
        pl.semaphore_signal(barrier, inc=1, device_id={"sp": sp + TEAM}, device_id_type=MESH)

    @pl.when(has_prev)
    def _():
        pl.semaphore_signal(barrier, inc=1, device_id={"sp": sp - TEAM}, device_id_type=MESH)

    row = lax.broadcasted_iota(jnp.int32, (tokens, tokens), 0)
    col = lax.broadcasted_iota(jnp.int32, (tokens, tokens), 1)
    for g in (1, 2):
        stride = STRIDES[g]
        each = tokens // stride
        origin = lax.rem(row, each) * stride + row // each
        perms[g - 1] = jnp.where(origin == col, 1.0, 0.0).astype(BF16)
    for g in range(3):
        stride = STRIDES[g]
        each = tokens // stride
        for r in range(stride):
            tables[0, g, r * each : (r + 1) * each, :] = cos_ref[pl.ds(r, each, stride=stride), :]
            tables[1, g, r * each : (r + 1) * each, :] = sin_ref[pl.ds(r, each, stride=stride), :]

    def prepare(kind, g):
        loads[kind, g].wait()

        def step(h, carry):
            lanes = pl.ds(pl.multiple_of(h * HEAD, HEAD), HEAD)
            x = raw[kind, g, :, lanes]
            if g > 0:
                x = jnp.dot(perms[g - 1], x, preferred_element_type=F32)
            else:
                x = x.astype(F32)
            if kind != V:
                x = x * tables[0, g] + pltpu.roll(x, HEAD // 2, 1) * tables[1, g]
            if kind == Q:
                x = x * HEAD ** (-0.5)
            ready[kind, g, :, lanes] = x.astype(BF16)
            return carry

        lax.fori_loop(0, heads, step, 0, unroll=2)

    def slot(kind, g, s):
        if kind == Q:
            return q_buf.at[g, s]
        if g == 2:
            return kv2.at[kind - 1, 2 * TEAM + s]
        if g == 1:
            return kv1.at[kind - 1, 2 + s]
        return kv0.at[kind - 1, pl.ds(pl.multiple_of(KEYS + s * tokens, KEYS), tokens)]

    def cols(head):
        return slice(head * HEAD, (head + 1) * HEAD)

    def lanes_of(j):
        return pl.ds(pl.multiple_of(j * part, part), part)

    def deal(kind, g, d):
        peer = lax.rem(me + d, TEAM)
        return pltpu.make_async_remote_copy(
            src_ref=ready.at[kind, g, :, lanes_of(peer)],
            dst_ref=slot(kind, g, me),
            send_sem=deal_send.at[kind, g, d],
            recv_sem=deal_recv.at[kind, g, d],
            device_id={"sp": team * TEAM + peer},
            device_id_type=MESH,
        )

    def source(d):
        return lax.rem(me + TEAM - d, TEAM)

    def wait_deal(kind, g, d):
        here = slot(kind, g, source(d))
        pltpu.make_async_remote_copy(
            src_ref=here, dst_ref=here,
            send_sem=deal_send.at[kind, g, d], recv_sem=deal_recv.at[kind, g, d],
            device_id={"sp": team * TEAM + source(d)}, device_id_type=MESH,
        ).wait_recv()

    near = TEAM * (1 + mine)

    def hop(kind, index, src, dst):
        return pltpu.make_async_remote_copy(
            src_ref=src, dst_ref=dst,
            send_sem=hop_send.at[kind - 1, index], recv_sem=hop_recv.at[kind - 1, index],
            device_id={"sp": lax.rem(sp + TEAM, n_sp)}, device_id_type=MESH,
        )

    def first_hop(kind, s):
        return hop(kind, s, kv2.at[kind - 1, 2 * TEAM + s], kv2.at[kind - 1, TEAM + s])

    def second_hop(kind, s, head):
        return hop(
            kind, TEAM * (1 + head) + s,
            kv2.at[kind - 1, TEAM + s, :, cols(head)], kv2.at[kind - 1, s, :, cols(head)],
        )

    def near_hop(kind, i):
        return hop(kind, near + i, kv1.at[kind - 1, TEAM + i], kv1.at[kind - 1, i])

    def edge_hop(kind):
        return hop(
            kind, near + 2,
            kv0.at[kind - 1, pl.ds(span, KEYS)], kv0.at[kind - 1, pl.ds(0, KEYS)],
        )

    def forward(kind, g, s):
        if g == 2:
            pl.when(has_next)(lambda: first_hop(kind, s).start())
        elif g == 1:
            pl.when(has_next & (s >= TEAM - 2))(lambda: near_hop(kind, s - (TEAM - 2)).start())
        else:
            pl.when(has_next & (s == TEAM - 1))(lambda: edge_hop(kind).start())

    def relay(d, head):
        s = source(d)
        for kind in (V, K):
            if head == 0:

                @pl.when(has_prev)
                def _():
                    first_hop(kind, s).wait_recv()

            @pl.when(has_prev & has_next)
            def _():
                second_hop(kind, s, head).start()

    def place(kind, g):
        slot(kind, g, me)[...] = ready[kind, g, :, lanes_of(me)]

    def arrive(g, d):
        for kind in (V, K):
            wait_deal(kind, g, d)
            forward(kind, g, source(d))

    barrier_waited = False
    for n, (kind, g) in enumerate(order):
        prepare(kind, g)
        place(kind, g)
        if not barrier_waited:
            count = TEAM + has_next.astype(jnp.int32) + has_prev.astype(jnp.int32)
            pl.semaphore_wait(barrier, count)
            barrier_waited = True
        for d in range(1, TEAM):
            deal(kind, g, d).start()
        if kind != Q:
            forward(kind, g, me)
        if n == 3:
            arrive(2, 1)
        if n == 5:
            arrive(2, 2)
    arrive(2, 3)
    relay(0, 0)
    relay(1, 0)
    for d in range(1, TEAM):
        arrive(1, d)
    relay(2, 0)
    relay(3, 0)
    for d in range(1, TEAM):
        arrive(0, d)
    for head in range(1, mine):
        for d in range(TEAM):
            relay(d, head)

    @pl.when(jnp.logical_not(has_prev))
    def _():
        for kind in range(2):
            kv0[kind, 0:KEYS, :] = jnp.zeros((KEYS, part), BF16)
            for s in range(2):
                kv1[kind, s] = jnp.zeros((tokens, part), BF16)
            for s in range(TEAM):
                kv2[kind, TEAM + s] = jnp.zeros((tokens, part), BF16)

    @pl.when(jnp.logical_not(has_prev2))
    def _():
        for kind in range(2):
            for s in range(TEAM):
                kv2[kind, s] = jnp.zeros((tokens, part), BF16)

    few = tokens // STRIDES[2]

    def fill(index, rows):
        a = lax.broadcasted_iota(jnp.int32, (rows, rows + KEYS), 0)
        b = lax.broadcasted_iota(jnp.int32, (rows, rows + KEYS), 1)
        allowed = (b >= jnp.maximum(a, KEYS - index)) & (b <= a + KEYS)
        return jnp.where(allowed, 0.0, MASKED)

    bias[0] = fill(team * span, KEYS)
    bias[1] = fill(KEYS, KEYS)
    bias[2, 0 : TEAM * few, 0 : TEAM * few + KEYS] = fill(team * TEAM * few, TEAM * few)

    def attend(g, head, query, key, value, off, start):
        rows = query.shape[0]
        scores = lax.dot_general(
            query, key, (((1,), (1,)), ((), ())), preferred_element_type=F32
        ) + off
        best = jnp.max(scores, axis=1, keepdims=True)
        weights = jnp.exp(scores - best)
        total = jnp.sum(weights, axis=1, keepdims=True)
        out = jnp.dot(weights.astype(BF16), value, preferred_element_type=F32) / total
        where = pl.ds(start, rows, stride=STRIDES[g]) if g else pl.ds(start, rows)
        acc[g, head, where, :] = out
        lse[g, head, where, :] = jnp.broadcast_to(best + jnp.log(total), (rows, HEAD))

    for d in range(1, TEAM):
        wait_deal(Q, 1, d)

    @pl.when(has_prev)
    def _():
        for kind in (V, K):
            for i in range(2):
                near_hop(kind, i).wait_recv()

    each = tokens // STRIDES[1]
    pair = KEYS // each

    def step1(n, carry):
        r, i = n // (TEAM // pair), lax.rem(n, TEAM // pair)
        rows = pl.ds(pl.multiple_of(r * each, each), each)
        for head in range(mine):
            query = q_buf[1, pl.ds(i * pair, pair), rows, cols(head)].reshape(KEYS, HEAD)
            key = kv1[0, pl.ds(i * pair, 2 * pair), rows, cols(head)].reshape(2 * KEYS, HEAD)
            value = kv1[1, pl.ds(i * pair, 2 * pair), rows, cols(head)].reshape(2 * KEYS, HEAD)
            attend(1, head, query, key, value,
                   bias[jnp.minimum(i, 1)], r + STRIDES[1] * KEYS * i)
        return carry

    lax.fori_loop(0, STRIDES[1] * (TEAM // pair), step1, 0, unroll=2)

    for d in range(1, TEAM):
        wait_deal(Q, 0, d)

    @pl.when(has_prev)
    def _():
        for kind in (V, K):
            edge_hop(kind).wait_recv()

    per = tokens // KEYS

    def step0(n, carry):
        inner = pl.ds(pl.multiple_of(lax.rem(n, per) * KEYS, KEYS), KEYS)
        rows = pl.ds(pl.multiple_of(n * KEYS, KEYS), 2 * KEYS)
        for head in range(mine):
            query = q_buf[0, n // per, inner, cols(head)]
            attend(0, head, query, kv0[0, rows, cols(head)], kv0[1, rows, cols(head)],
                   bias[jnp.minimum(n, 1)], pl.multiple_of(n * KEYS, KEYS))
        return carry

    lax.fori_loop(0, span // KEYS, step0, 0, unroll=2)

    for d in range(1, TEAM):
        wait_deal(Q, 2, d)

    def far(head):
        def step(r, carry):
            rows = pl.ds(pl.multiple_of(r * few, few), few)
            query = q_buf[2, :, rows, cols(head)].reshape(TEAM * few, HEAD)
            key = kv2[0, :, rows, cols(head)].reshape(3 * TEAM * few, HEAD)
            value = kv2[1, :, rows, cols(head)].reshape(3 * TEAM * few, HEAD)
            attend(2, head, query, key, value, bias[2, 0 : TEAM * few, 0 : TEAM * few + KEYS], r)
            return carry

        lax.fori_loop(0, STRIDES[2], step, 0, unroll=4)

    def merge(j, head):
        rows = pl.ds(pl.multiple_of(j * tokens, tokens), tokens)
        logs = [lse[g, head, rows, :] for g in range(3)]
        peak = jnp.maximum(jnp.maximum(logs[0], logs[1]), logs[2])
        upper = jnp.zeros((tokens, HEAD), F32)
        lower = jnp.zeros((tokens, HEAD), F32)
        for g in range(3):
            scale = jnp.exp(logs[g] - peak)
            upper = upper + scale * acc[g, head, rows, :]
            lower = lower + scale
        att[head, j] = (upper / lower).astype(BF16)

    def place_of(s):
        return pl.ds(pl.multiple_of(s * HEAD, HEAD), HEAD)

    def home(d, head):
        peer = lax.rem(me + d, TEAM)
        return pltpu.make_async_remote_copy(
            src_ref=att.at[head, peer], dst_ref=full.at[tp, head, :, place_of(me)],
            send_sem=ret_send.at[d, head], recv_sem=ret_recv.at[d, head],
            device_id={"sp": team * TEAM + peer}, device_id_type=MESH,
        )

    def wait_home(d, head):
        here = full.at[tp, head, :, place_of(source(d))]
        pltpu.make_async_remote_copy(
            src_ref=here, dst_ref=here,
            send_sem=ret_send.at[d, head], recv_sem=ret_recv.at[d, head],
            device_id={"sp": team * TEAM + source(d)}, device_id_type=MESH,
        ).wait_recv()

    def twin(d, half, head):
        here = full.at[half, head, :, place_of(source(d))]
        return pltpu.make_async_remote_copy(
            src_ref=here, dst_ref=here,
            send_sem=d2d_send.at[d, head], recv_sem=d2d_recv.at[d, head],
            device_id={"tp": 1 - tp}, device_id_type=MESH,
        )

    for copy in w_loads:
        copy.wait()
    for head in range(mine):

        @pl.when(has_prev2)
        def _():
            for d in range(TEAM):
                for kind in (V, K):
                    second_hop(kind, source(d), head).wait_recv()

        far(head)
        for d in (2, 1, 3, 0):
            merge(lax.rem(me + d, TEAM), head)
            if d:
                home(d, head).start()
        full[tp, head, :, place_of(me)] = att[head, me]
        twin(0, tp, head).start()
        for d in (1, 3, 2):
            wait_home(d, head)
            twin(d, tp, head).start()
        product = jnp.dot(full[tp, head], w_buf[tp, head], preferred_element_type=F32)
        for d in range(TEAM):
            twin(d, 1 - tp, head).wait_recv()
        product = product + jnp.dot(
            full[1 - tp, head], w_buf[1 - tp, head], preferred_element_type=F32
        )
        if head == 0:
            total_buf[...] = product
        elif head < mine - 1:
            total_buf[...] += product
        else:
            o_ref[...] = (total_buf[...] + product).astype(BF16)

    for kind, g in order:
        for d in range(1, TEAM):
            deal(kind, g, d).wait_send()
    for head in range(mine):
        for d in range(1, TEAM):
            home(d, head).wait_send()
        for d in range(TEAM):
            twin(d, tp, head).wait_send()

    @pl.when(has_next)
    def _():
        for kind in (V, K):
            for s in range(TEAM):
                first_hop(kind, s).wait_send()
            for i in range(2):
                near_hop(kind, i).wait_send()
            edge_hop(kind).wait_send()

    @pl.when(has_prev & has_next)
    def _():
        for kind in (V, K):
            for s in range(TEAM):
                for head in range(mine):
                    second_hop(kind, s, head).wait_send()


def shards(n_sp, queries, keys, values, w_out):
    tokens, width = queries.shape[1:]
    heads = width // HEAD
    mine = heads // TEAM
    part = mine * HEAD
    span = TEAM * tokens
    start = lax.axis_index("sp") * tokens
    positions = (lax.iota(jnp.int32, tokens) + start).astype(F32)
    inverse = ROPE_BASE ** (-jnp.arange(0, HEAD, 2, dtype=F32) / HEAD)
    angles = positions[:, None] * inverse[None, :]
    cosine, sine = jnp.cos(angles), jnp.sin(angles)
    cosine = jnp.concatenate([cosine, cosine], axis=1)
    sine = jnp.concatenate([-sine, sine], axis=1)
    any_spec = pl.BlockSpec(memory_space=pl.ANY)
    vmem = pl.BlockSpec(memory_space=pltpu.VMEM)
    dma = pltpu.SemaphoreType.DMA
    return pl.pallas_call(
        functools.partial(kernel, (tokens, n_sp, heads)),
        out_shape=jax.ShapeDtypeStruct((tokens, w_out.shape[1]), BF16),
        in_specs=[any_spec] * 4 + [vmem] * 2,
        out_specs=vmem,
        scratch_shapes=[
            pltpu.VMEM((3, 3, tokens, width), BF16),
            pltpu.VMEM((3, 3, tokens, width), BF16),
            pltpu.VMEM((2, mine, TEAM * HEAD, w_out.shape[1]), BF16),
            pltpu.VMEM((2, 3, tokens, HEAD), F32),
            pltpu.VMEM((2, tokens, tokens), BF16),
            pltpu.VMEM((3, TEAM, tokens, part), BF16),
            pltpu.VMEM((2, KEYS + span, part), BF16),
            pltpu.VMEM((2, 2 + TEAM, tokens, part), BF16),
            pltpu.VMEM((2, 3 * TEAM, tokens, part), BF16),
            pltpu.VMEM((3, mine, span, HEAD), F32),
            pltpu.VMEM((3, mine, span, HEAD), F32),
            pltpu.VMEM((3, KEYS, 2 * KEYS), F32),
            pltpu.VMEM((mine, TEAM, tokens, HEAD), BF16),
            pltpu.VMEM((2, mine, tokens, TEAM * HEAD), BF16),
            pltpu.VMEM((tokens, w_out.shape[1]), F32),
            dma((3, 3)),
            dma((2, mine, TEAM)),
            dma((3, 3, TEAM)),
            dma((3, 3, TEAM)),
            dma((2, TEAM * (1 + mine) + 3)),
            dma((2, TEAM * (1 + mine) + 3)),
            dma((TEAM, mine)),
            dma((TEAM, mine)),
            dma((TEAM, mine)),
            dma((TEAM, mine)),
        ],
        compiler_params=pltpu.CompilerParams(
            collective_id=0, has_side_effects=True, vmem_limit_bytes=60 * 1024 * 1024
        ),
    )(queries, keys, values, w_out, cosine, sine)


def solution(mesh):
    return jax.shard_map(
        functools.partial(shards, mesh.shape["sp"]),
        mesh=mesh,
        in_specs=(P(None, "sp", "tp"), P(None, "sp", "tp"), P(None, "sp", "tp"), P(None, "tp")),
        out_specs=P("sp", "tp"),
        check_vma=False,
    )
```

```python
import functools

import jax
import jax.numpy as jnp
from jax import lax
from jax.experimental import pallas as pl
from jax.experimental.pallas import tpu as pltpu
from jax.sharding import PartitionSpec as P

HEAD = 128
KEYS = 128
STRIDES = (1, 4, 16)
ROPE_BASE = 10000.0
MASKED = -1e30
TEAM = 4

MESH = pl.DeviceIdType.MESH
F32 = jnp.float32
BF16 = jnp.bfloat16


def kernel(
    cfg,
    q_in, k_in, v_in, w_in, cos_ref, sin_ref,
    o_ref,
    raw, ready, w_buf, tables, perms, q_buf, kv0, kv1, kv2, acc, lse, bias, att, full, total_buf,
    in_sem, w_sem, deal_send, deal_recv, hop_send, hop_recv, ret_send, ret_recv, d2d_send, d2d_recv,
):
    tokens, n_sp, heads = cfg
    width = heads * HEAD
    mine = heads // TEAM
    part = mine * HEAD
    span = TEAM * tokens
    sp = lax.axis_index("sp")
    tp = lax.axis_index("tp")
    team = sp // TEAM
    me = lax.rem(sp, TEAM)
    has_next = sp + TEAM < n_sp
    has_prev = sp >= TEAM
    has_prev2 = sp >= 2 * TEAM

    inputs = (q_in, k_in, v_in)
    Q, K, V = 0, 1, 2
    order = [(V, 2), (K, 2), (V, 1), (K, 1), (V, 0), (K, 0), (Q, 2), (Q, 1), (Q, 0)]
    loads = {}
    for kind, g in order:
        copy = pltpu.make_async_copy(inputs[kind].at[g], raw.at[kind, g], in_sem.at[kind, g])
        copy.start()
        loads[kind, g] = copy
    w_loads = []
    for half in range(2):
        for head in range(mine):
            for s in range(TEAM):
                rows = pl.ds(half * width + s * part + head * HEAD, HEAD)
                copy = pltpu.make_async_copy(
                    w_in.at[rows],
                    w_buf.at[half, head, pl.ds(s * HEAD, HEAD)],
                    w_sem.at[half, head, s],
                )
                copy.start()
                w_loads.append(copy)

    barrier = pltpu.get_barrier_semaphore()
    for d in range(1, TEAM):
        peer = team * TEAM + lax.rem(me + d, TEAM)
        pl.semaphore_signal(barrier, inc=1, device_id={"sp": peer}, device_id_type=MESH)
    pl.semaphore_signal(barrier, inc=1, device_id={"tp": 1 - tp}, device_id_type=MESH)

    @pl.when(has_next)
    def _():
        pl.semaphore_signal(barrier, inc=1, device_id={"sp": sp + TEAM}, device_id_type=MESH)

    @pl.when(has_prev)
    def _():
        pl.semaphore_signal(barrier, inc=1, device_id={"sp": sp - TEAM}, device_id_type=MESH)

    row = lax.broadcasted_iota(jnp.int32, (tokens, tokens), 0)
    col = lax.broadcasted_iota(jnp.int32, (tokens, tokens), 1)

    def sorter(g):
        each = tokens // STRIDES[g]
        origin = lax.rem(row, each) * STRIDES[g] + row // each
        perms[g - 1] = jnp.where(origin == col, 1.0, 0.0).astype(BF16)

    def sort_tables(g):
        stride = STRIDES[g]
        each = tokens // stride
        for r in range(stride):
            tables[0, g, r * each : (r + 1) * each, :] = cos_ref[pl.ds(r, each, stride=stride), :]
            tables[1, g, r * each : (r + 1) * each, :] = sin_ref[pl.ds(r, each, stride=stride), :]

    def prepare(kind, g):
        loads[kind, g].wait()

        def step(h, carry):
            lanes = pl.ds(pl.multiple_of(h * HEAD, HEAD), HEAD)
            x = raw[kind, g, :, lanes]
            if g > 0:
                x = jnp.dot(perms[g - 1], x, preferred_element_type=F32)
            else:
                x = x.astype(F32)
            if kind != V:
                x = x * tables[0, g] + pltpu.roll(x, HEAD // 2, 1) * tables[1, g]
            if kind == Q:
                x = x * HEAD ** (-0.5)
            ready[kind, g, :, lanes] = x.astype(BF16)
            return carry

        lax.fori_loop(0, heads, step, 0, unroll=2)

    def slot(kind, g, s):
        if kind == Q:
            return q_buf.at[g, s]
        if g == 2:
            return kv2.at[kind - 1, 2 * TEAM + s]
        if g == 1:
            return kv1.at[kind - 1, 2 + s]
        return kv0.at[kind - 1, pl.ds(pl.multiple_of(KEYS + s * tokens, KEYS), tokens)]

    def cols(head):
        return slice(head * HEAD, (head + 1) * HEAD)

    def lanes_of(j):
        return pl.ds(pl.multiple_of(j * part, part), part)

    def deal(kind, g, d):
        peer = lax.rem(me + d, TEAM)
        return pltpu.make_async_remote_copy(
            src_ref=ready.at[kind, g, :, lanes_of(peer)],
            dst_ref=slot(kind, g, me),
            send_sem=deal_send.at[kind, g, d],
            recv_sem=deal_recv.at[kind, g, d],
            device_id={"sp": team * TEAM + peer},
            device_id_type=MESH,
        )

    def source(d):
        return lax.rem(me + TEAM - d, TEAM)

    def wait_deal(kind, g, d):
        here = slot(kind, g, source(d))
        pltpu.make_async_remote_copy(
            src_ref=here, dst_ref=here,
            send_sem=deal_send.at[kind, g, d], recv_sem=deal_recv.at[kind, g, d],
            device_id={"sp": team * TEAM + source(d)}, device_id_type=MESH,
        ).wait_recv()

    near = TEAM * (1 + mine)

    def hop(kind, index, src, dst):
        return pltpu.make_async_remote_copy(
            src_ref=src, dst_ref=dst,
            send_sem=hop_send.at[kind - 1, index], recv_sem=hop_recv.at[kind - 1, index],
            device_id={"sp": lax.rem(sp + TEAM, n_sp)}, device_id_type=MESH,
        )

    def first_hop(kind, s):
        return hop(kind, s, kv2.at[kind - 1, 2 * TEAM + s], kv2.at[kind - 1, TEAM + s])

    def second_hop(kind, s, head):
        return hop(
            kind, TEAM * (1 + head) + s,
            kv2.at[kind - 1, TEAM + s, :, cols(head)], kv2.at[kind - 1, s, :, cols(head)],
        )

    def near_hop(kind, i):
        return hop(kind, near + i, kv1.at[kind - 1, TEAM + i], kv1.at[kind - 1, i])

    def edge_hop(kind):
        return hop(
            kind, near + 2,
            kv0.at[kind - 1, pl.ds(span, KEYS)], kv0.at[kind - 1, pl.ds(0, KEYS)],
        )

    def forward(kind, g, s):
        if g == 2:
            pl.when(has_next)(lambda: first_hop(kind, s).start())
        elif g == 1:
            pl.when(has_next & (s >= TEAM - 2))(lambda: near_hop(kind, s - (TEAM - 2)).start())
        else:
            pl.when(has_next & (s == TEAM - 1))(lambda: edge_hop(kind).start())

    def relay(d, head):
        s = source(d)
        for kind in (V, K):
            if head == 0:

                @pl.when(has_prev)
                def _():
                    first_hop(kind, s).wait_recv()

            @pl.when(has_prev & has_next)
            def _():
                second_hop(kind, s, head).start()

    def place(kind, g):
        slot(kind, g, me)[...] = ready[kind, g, :, lanes_of(me)]

    def arrive(g, d):
        for kind in (V, K):
            wait_deal(kind, g, d)
            forward(kind, g, source(d))

    barrier_waited = False
    for n, (kind, g) in enumerate(order):
        if kind == V and g > 0:
            sorter(g)
        if kind == K:
            sort_tables(g)
        prepare(kind, g)
        place(kind, g)
        if not barrier_waited:
            count = TEAM + has_next.astype(jnp.int32) + has_prev.astype(jnp.int32)
            pl.semaphore_wait(barrier, count)
            barrier_waited = True
        for d in range(1, TEAM):
            deal(kind, g, d).start()
        if kind != Q:
            forward(kind, g, me)
        if n == 3:
            arrive(2, 1)
        if n == 5:
            arrive(2, 2)
    arrive(2, 3)
    relay(0, 0)
    relay(1, 0)
    for d in range(1, TEAM):
        arrive(1, d)
    relay(2, 0)
    relay(3, 0)
    for d in range(1, TEAM):
        arrive(0, d)
    for head in range(1, mine):
        for d in range(TEAM):
            relay(d, head)

    @pl.when(jnp.logical_not(has_prev))
    def _():
        for kind in range(2):
            kv0[kind, 0:KEYS, :] = jnp.zeros((KEYS, part), BF16)
            for s in range(2):
                kv1[kind, s] = jnp.zeros((tokens, part), BF16)
            for s in range(TEAM):
                kv2[kind, TEAM + s] = jnp.zeros((tokens, part), BF16)

    @pl.when(jnp.logical_not(has_prev2))
    def _():
        for kind in range(2):
            for s in range(TEAM):
                kv2[kind, s] = jnp.zeros((tokens, part), BF16)

    few = tokens // STRIDES[2]

    def fill(index, rows):
        a = lax.broadcasted_iota(jnp.int32, (rows, rows + KEYS), 0)
        b = lax.broadcasted_iota(jnp.int32, (rows, rows + KEYS), 1)
        allowed = (b >= jnp.maximum(a, KEYS - index)) & (b <= a + KEYS)
        return jnp.where(allowed, 0.0, MASKED)

    bias[0] = fill(team * span, KEYS)
    bias[1] = fill(KEYS, KEYS)
    bias[2, 0 : TEAM * few, 0 : TEAM * few + KEYS] = fill(team * TEAM * few, TEAM * few)

    def attend(g, tiles):
        scores = [
            lax.dot_general(t[1], t[2], (((1,), (1,)), ((), ())), preferred_element_type=F32)
            + t[4]
            for t in tiles
        ]
        best = [jnp.max(x, axis=1, keepdims=True) for x in scores]
        weights = [jnp.exp(x - m) for x, m in zip(scores, best)]
        outs = [
            jnp.dot(p.astype(BF16), t[3], preferred_element_type=F32)
            for p, t in zip(weights, tiles)
        ]
        total = [jnp.sum(p, axis=1, keepdims=True) for p in weights]
        for t, out, m, l in zip(tiles, outs, best, total):
            rows = out.shape[0]
            where = pl.ds(t[5], rows, stride=STRIDES[g]) if g else pl.ds(t[5], rows)
            acc[g, t[0], where, :] = out / l
            lse[g, t[0], where, :] = jnp.broadcast_to(m + jnp.log(l), (rows, HEAD))

    def far(head):
        @pl.when(has_prev2)
        def _():
            for d in range(TEAM):
                for kind in (V, K):
                    second_hop(kind, source(d), head).wait_recv()

        off = bias[2, 0 : TEAM * few, 0 : TEAM * few + KEYS]
        for first in range(0, STRIDES[2], 4):
            tiles = []
            for r in range(first, first + 4):
                rows = slice(r * few, (r + 1) * few)
                query = q_buf[2, :, rows, cols(head)].reshape(TEAM * few, HEAD)
                key = kv2[0, :, rows, cols(head)].reshape(3 * TEAM * few, HEAD)
                value = kv2[1, :, rows, cols(head)].reshape(3 * TEAM * few, HEAD)
                tiles.append((head, query, key, value, off, r))
            attend(2, tiles)

    for d in range(1, TEAM):
        wait_deal(Q, 2, d)
    far(0)

    for d in range(1, TEAM):
        wait_deal(Q, 1, d)

    @pl.when(has_prev)
    def _():
        for kind in (V, K):
            for i in range(2):
                near_hop(kind, i).wait_recv()

    each = tokens // STRIDES[1]
    pair = KEYS // each

    def step1(n, carry):
        r, i = n // (TEAM // pair), lax.rem(n, TEAM // pair)
        rows = pl.ds(pl.multiple_of(r * each, each), each)
        tiles = []
        for head in range(mine):
            query = q_buf[1, pl.ds(i * pair, pair), rows, cols(head)].reshape(KEYS, HEAD)
            key = kv1[0, pl.ds(i * pair, 2 * pair), rows, cols(head)].reshape(2 * KEYS, HEAD)
            value = kv1[1, pl.ds(i * pair, 2 * pair), rows, cols(head)].reshape(2 * KEYS, HEAD)
            tiles.append((head, query, key, value,
                          bias[jnp.minimum(i, 1)], r + STRIDES[1] * KEYS * i))
        attend(1, tiles)
        return carry

    lax.fori_loop(0, STRIDES[1] * (TEAM // pair), step1, 0, unroll=2)

    for d in range(1, TEAM):
        wait_deal(Q, 0, d)

    @pl.when(has_prev)
    def _():
        for kind in (V, K):
            edge_hop(kind).wait_recv()

    per = tokens // KEYS

    def step0(n, carry):
        inner = pl.ds(pl.multiple_of(lax.rem(n, per) * KEYS, KEYS), KEYS)
        rows = pl.ds(pl.multiple_of(n * KEYS, KEYS), 2 * KEYS)
        tiles = []
        for head in range(mine):
            query = q_buf[0, n // per, inner, cols(head)]
            tiles.append((head, query, kv0[0, rows, cols(head)], kv0[1, rows, cols(head)],
                          bias[jnp.minimum(n, 1)], pl.multiple_of(n * KEYS, KEYS)))
        attend(0, tiles)
        return carry

    lax.fori_loop(0, span // KEYS, step0, 0, unroll=2)

    def merge(j, head):
        rows = pl.ds(pl.multiple_of(j * tokens, tokens), tokens)
        logs = [lse[g, head, rows, :] for g in range(3)]
        peak = jnp.maximum(jnp.maximum(logs[0], logs[1]), logs[2])
        upper = jnp.zeros((tokens, HEAD), F32)
        lower = jnp.zeros((tokens, HEAD), F32)
        for g in range(3):
            scale = jnp.exp(logs[g] - peak)
            upper = upper + scale * acc[g, head, rows, :]
            lower = lower + scale
        att[head, j] = (upper / lower).astype(BF16)

    def place_of(s):
        return pl.ds(pl.multiple_of(s * HEAD, HEAD), HEAD)

    def home(d, head):
        peer = lax.rem(me + d, TEAM)
        return pltpu.make_async_remote_copy(
            src_ref=att.at[head, peer], dst_ref=full.at[tp, head, :, place_of(me)],
            send_sem=ret_send.at[d, head], recv_sem=ret_recv.at[d, head],
            device_id={"sp": team * TEAM + peer}, device_id_type=MESH,
        )

    def wait_home(d, head):
        here = full.at[tp, head, :, place_of(source(d))]
        pltpu.make_async_remote_copy(
            src_ref=here, dst_ref=here,
            send_sem=ret_send.at[d, head], recv_sem=ret_recv.at[d, head],
            device_id={"sp": team * TEAM + source(d)}, device_id_type=MESH,
        ).wait_recv()

    def twin(d, half, head):
        here = full.at[half, head, :, place_of(source(d))]
        return pltpu.make_async_remote_copy(
            src_ref=here, dst_ref=here,
            send_sem=d2d_send.at[d, head], recv_sem=d2d_recv.at[d, head],
            device_id={"tp": 1 - tp}, device_id_type=MESH,
        )

    for copy in w_loads:
        copy.wait()
    for head in range(mine):
        if head:
            far(head)
        for d in (2, 1, 3, 0):
            merge(lax.rem(me + d, TEAM), head)
            if d:
                home(d, head).start()
        full[tp, head, :, place_of(me)] = att[head, me]
        twin(0, tp, head).start()
    for head in range(mine):
        for d in (1, 3, 2):
            wait_home(d, head)
            twin(d, tp, head).start()
        product = jnp.dot(full[tp, head], w_buf[tp, head], preferred_element_type=F32)
        for d in range(TEAM):
            twin(d, 1 - tp, head).wait_recv()
        product = product + jnp.dot(
            full[1 - tp, head], w_buf[1 - tp, head], preferred_element_type=F32
        )
        if head == 0:
            total_buf[...] = product
        elif head < mine - 1:
            total_buf[...] += product
        else:
            o_ref[...] = (total_buf[...] + product).astype(BF16)

    for kind, g in order:
        for d in range(1, TEAM):
            deal(kind, g, d).wait_send()
    for head in range(mine):
        for d in range(1, TEAM):
            home(d, head).wait_send()
        for d in range(TEAM):
            twin(d, tp, head).wait_send()

    @pl.when(has_next)
    def _():
        for kind in (V, K):
            for s in range(TEAM):
                first_hop(kind, s).wait_send()
            for i in range(2):
                near_hop(kind, i).wait_send()
            edge_hop(kind).wait_send()

    @pl.when(has_prev & has_next)
    def _():
        for kind in (V, K):
            for s in range(TEAM):
                for head in range(mine):
                    second_hop(kind, s, head).wait_send()


def shards(n_sp, queries, keys, values, w_out):
    tokens, width = queries.shape[1:]
    heads = width // HEAD
    mine = heads // TEAM
    part = mine * HEAD
    span = TEAM * tokens
    start = lax.axis_index("sp") * tokens
    positions = (lax.iota(jnp.int32, tokens) + start).astype(F32)
    inverse = ROPE_BASE ** (-jnp.arange(0, HEAD, 2, dtype=F32) / HEAD)
    angles = positions[:, None] * inverse[None, :]
    cosine, sine = jnp.cos(angles), jnp.sin(angles)
    cosine = jnp.concatenate([cosine, cosine], axis=1)
    sine = jnp.concatenate([-sine, sine], axis=1)
    any_spec = pl.BlockSpec(memory_space=pl.ANY)
    vmem = pl.BlockSpec(memory_space=pltpu.VMEM)
    dma = pltpu.SemaphoreType.DMA
    return pl.pallas_call(
        functools.partial(kernel, (tokens, n_sp, heads)),
        out_shape=jax.ShapeDtypeStruct((tokens, w_out.shape[1]), BF16),
        in_specs=[any_spec] * 4 + [vmem] * 2,
        out_specs=vmem,
        scratch_shapes=[
            pltpu.VMEM((3, 3, tokens, width), BF16),
            pltpu.VMEM((3, 3, tokens, width), BF16),
            pltpu.VMEM((2, mine, TEAM * HEAD, w_out.shape[1]), BF16),
            pltpu.VMEM((2, 3, tokens, HEAD), F32),
            pltpu.VMEM((2, tokens, tokens), BF16),
            pltpu.VMEM((3, TEAM, tokens, part), BF16),
            pltpu.VMEM((2, KEYS + span, part), BF16),
            pltpu.VMEM((2, 2 + TEAM, tokens, part), BF16),
            pltpu.VMEM((2, 3 * TEAM, tokens, part), BF16),
            pltpu.VMEM((3, mine, span, HEAD), F32),
            pltpu.VMEM((3, mine, span, HEAD), F32),
            pltpu.VMEM((3, KEYS, 2 * KEYS), F32),
            pltpu.VMEM((mine, TEAM, tokens, HEAD), BF16),
            pltpu.VMEM((2, mine, tokens, TEAM * HEAD), BF16),
            pltpu.VMEM((tokens, w_out.shape[1]), F32),
            dma((3, 3)),
            dma((2, mine, TEAM)),
            dma((3, 3, TEAM)),
            dma((3, 3, TEAM)),
            dma((2, TEAM * (1 + mine) + 3)),
            dma((2, TEAM * (1 + mine) + 3)),
            dma((TEAM, mine)),
            dma((TEAM, mine)),
            dma((TEAM, mine)),
            dma((TEAM, mine)),
        ],
        compiler_params=pltpu.CompilerParams(
            collective_id=0, has_side_effects=True, vmem_limit_bytes=60 * 1024 * 1024
        ),
    )(queries, keys, values, w_out, cosine, sine)


def solution(mesh):
    return jax.shard_map(
        functools.partial(shards, mesh.shape["sp"]),
        mesh=mesh,
        in_specs=(P(None, "sp", "tp"), P(None, "sp", "tp"), P(None, "sp", "tp"), P(None, "tp")),
        out_specs=P("sp", "tp"),
        check_vma=False,
    )
```
